32 devices in a mesh: ep: 4 (over y, x), tp: 8 (over z, core).
Axes of the slice: x: 2, y: 2, z: 4, core: 2. Of those that a mesh axis runs over, the one named last changes fastest.
Arguments:
- mixer_input: bfloat16 [6144, 1024], P(('ep', 'tp')), may hold values from -6 to 6
- mixer_gain: float32 [1024], replicated, may hold values from 0.1 to 1.9
- group_weight: bfloat16 [4, 256, 256], replicated, may hold values from -0.375 to 0.375
- mixer_scale: float32 [1024], replicated, may hold values from 0.1 to 1.9
- expert_input: bfloat16 [6144, 1024], P(('ep', 'tp')), may hold values from -6 to 6
- expert_gain: float32 [1024], replicated, may hold values from 0.1 to 1.9
- routes: int32 [6144, 2], P(('ep', 'tp')), may hold values from 0 to 3, all different within a row; in each aligned block of 192 rows (0 to 191, 192 to 383, ...) at most 144 rows name the same one
- route_weight: float32 [6144, 2], P(('ep', 'tp')), may hold values from 0.2 to 1
- w_gate: bfloat16 [4, 1024, 4096], P('ep', None, 'tp'), may hold values from -0.1875 to 0.1875
- w_up: bfloat16 [4, 1024, 4096], P('ep', None, 'tp'), may hold values from -0.1875 to 0.1875
- w_down: bfloat16 [4, 4096, 1024], P('ep', 'tp'), may hold values from -0.09375 to 0.09375
Outputs:
- mixer_out: bfloat16 [6144, 1024], P(('ep', 'tp'))
- expert_out: bfloat16 [6144, 1024], P(('ep', 'tp'))
The draws below stay inside these ranges and needn't reach their ends.
Inputs may be any that keep to these rules, and one draw needn't show every extreme that they name: `routes`: each row names 2 different experts. Among the rows of one device no expert is named by more than 144 rows, and in some device's rows some expert is named exactly 144 times.
All inputs are finite; a program needn't handle non-finite values.
Results may differ from the reference program's by a relative error of at most 0.0076.
Values may be sent and summed in bfloat16 or wider, within the bound.
A program may use at most 128 MiB of HBM per device.

```python
import math
import jax
import jax.numpy as jnp
import numpy as np
from jax import lax

D = 1024
GROUP_WIDTH = 256
FFE = 4096
TOPK = 2
TOK_DEV = 192
EXPERTS = 4
CAP = 144
TOKENS = 6144
N_TP = 8
DEVICES = 32


def block_levels(rng, dims, pieces, low, largest):
    factor_of = 1.0
    for dim, blocks in pieces:
        heights = jax.random.uniform(jax.random.fold_in(jax.random.fold_in(rng, 6), dim), (blocks,), jnp.float32, low / len(pieces), largest / len(pieces))
        factor_of = factor_of * jnp.repeat(jnp.exp(heights), dims[dim] // blocks).reshape((-1,) + (1,) * (len(dims) - 1 - dim))
    return factor_of


def deal_out(own_key, own, number, rows, amount, top, bound, lean):
    ranking = jax.random.permutation(own_key, amount)
    crowded, ordinary = shares(amount, rows * top, bound, lean, True), shares(amount, rows * top, bound, lean, False)
    places = jnp.arange(amount)

    def named(tallies, turn):
        used = int((tallies > 0).sum())
        fixed = max(1, used // 4)
        passed = fixed + (places - fixed + turn * (used - fixed)) % max(1, amount - fixed)
        return jnp.zeros((amount,), jnp.int32).at[ranking[jnp.where(places < fixed, places, passed)]].set(jnp.asarray(tallies, jnp.int32))

    tallies = jnp.where(number % 4 == 0, named(crowded, number // 4), named(ordinary, number - number // 4 - 1))
    mixed = jax.random.permutation(jax.random.fold_in(own, 3), amount)
    giver, taker = mixed[0:amount // 2 * 2:2], mixed[1:amount // 2 * 2:2]
    room = jnp.minimum(tallies[giver] - 1, bound - tallies[taker]) // 2
    room = jnp.where((giver == ranking[0]) | (taker == ranking[0]) | (tallies[taker] == 0), 0, jnp.maximum(room, 0))
    passed = jax.random.randint(jax.random.fold_in(own, 4), (amount // 2,), 0, 1 << 20) % (room + 1)
    tallies = tallies.at[giver].add(-passed).at[taker].add(passed)
    labels = jnp.searchsorted(jnp.cumsum(tallies), jnp.arange(rows * top), side="right").astype(jnp.int32)
    listing = labels.reshape(top, rows).T
    listing = listing[jax.random.permutation(jax.random.fold_in(own, 1), rows)]
    turn = jax.random.randint(jax.random.fold_in(own, 2), (rows, 1), 0, top)
    return jnp.take_along_axis(listing, (jnp.arange(top)[None, :] + turn) % top, axis=1)


def shares(count, total, most, lean, full):
    portions = [(1 << 20) // math.isqrt(rank ** lean) + 1 for rank in range(1, count + 1)]
    largest = most if full else min(most, max(-(-total // count), total * portions[0] // sum(portions)))
    least = 1 if total - largest >= count - 1 else 0
    given, spare = [largest] + [least] * (count - 1), total - largest - least * (count - 1)
    while spare > 0:
        free = [i for i in range(1, count) if given[i] < largest] or [i for i in range(1, count) if given[i] < most]
        pool, budget = sum([portions[i] for i in free]), spare
        for i in free:
            more = min(most - given[i], max(1, budget * portions[i] // pool), spare)
            given[i] = given[i] + more
            spare = spare - more
    return np.array(given)


def normal_values(stream_key, dims, width, bound, shards=(), kind=jnp.bfloat16):
    values = jax.random.normal(stream_key, dims, jnp.float32) * width
    if len(shards) > 0:
        values = block_levels(stream_key, dims, shards, -0.22, 0.18) * values
    return jnp.clip(values, min=-bound, max=bound).astype(kind)


def setup_inputs(seed: int = 0) -> dict:
    key_of = jax.random.split(jax.random.key(seed), 12)
    mixer_input = normal_values(key_of[0], (TOKENS, D), 1.0, 6.0, ((0, 32),))
    mixer_gain = jnp.clip(1.0 + 0.18 * jax.random.normal(key_of[1], (D,), jnp.float32), 0.1, 1.9)
    group_weight = normal_values(key_of[2], (4, GROUP_WIDTH, GROUP_WIDTH), GROUP_WIDTH ** -0.5, 0.375)
    mixer_scale = jnp.clip(1.0 + 0.18 * jax.random.normal(key_of[3], (D,), jnp.float32), 0.1, 1.9)
    expert_input = normal_values(key_of[4], (TOKENS, D), 1.0, 6.0, ((0, 32),))
    expert_gain = jnp.clip(1.0 + 0.18 * jax.random.normal(key_of[5], (D,), jnp.float32), 0.1, 1.9)
    routes_keys = jax.random.split(jax.random.fold_in(key_of[6], 1), TOKENS // TOK_DEV)
    routes_turns = jax.random.permutation(jax.random.fold_in(key_of[6], 3), TOKENS // TOK_DEV)
    routes = jax.vmap(lambda own, number: deal_out(jax.random.fold_in(key_of[6], 2), own, number, TOK_DEV, EXPERTS, TOPK, CAP, 2))(routes_keys, routes_turns).reshape((TOKENS, TOPK))
    route_weight = jnp.clip(0.2 + 0.8 * jax.random.uniform(key_of[7], (TOKENS, TOPK), jnp.float32) ** block_levels(key_of[7], (TOKENS, TOPK), ((0, 32),), -0.2, 0.2), 0.2, 1.0)
    w_gate = normal_values(key_of[8], (EXPERTS, D, FFE), D ** -0.5, 0.1875, ((0, 4), (2, 8)))
    w_up = normal_values(key_of[9], (EXPERTS, D, FFE), D ** -0.5, 0.1875, ((0, 4), (2, 8)))
    w_down = normal_values(key_of[10], (EXPERTS, FFE, D), FFE ** -0.5, 0.09375, ((0, 4), (1, 8)))
    return dict(mixer_input=mixer_input, mixer_gain=mixer_gain, group_weight=group_weight, mixer_scale=mixer_scale, expert_input=expert_input, expert_gain=expert_gain, routes=routes, route_weight=route_weight, w_gate=w_gate, w_up=w_up, w_down=w_down)


epsilon = 1e-06

def normalize(row_values, gain):
    values = row_values.astype(jnp.float32)
    scaled = values * lax.rsqrt(lax.optimization_barrier(jnp.mean(values * values, axis=-1, keepdims=True)) + epsilon)
    return (scaled * gain).astype(jnp.bfloat16)

def pool_groups(padded, start_row, row_count, seq_length):
    group_width = padded.shape[1] // 4
    position = start_row + jnp.arange(row_count, dtype=jnp.int32)
    centre = padded[8:8 + row_count]
    pooled_parts = []
    for group_index in range(4):
        window = 2 ** (group_index + 1)
        reach_left = window // 2
        reach_right = window - 1 - reach_left
        group_cols = padded[:, group_index * group_width:(group_index + 1) * group_width]
        window_sum = group_cols[8 - reach_left:8 - reach_left + row_count]
        for offset in range(1 - reach_left, reach_right + 1):
            window_sum = window_sum + group_cols[8 + offset:8 + offset + row_count]
        cover = (jnp.minimum(position + reach_right + 1, seq_length) - jnp.maximum(position - reach_left, 0)).astype(jnp.float32)
        pooled_parts.append(window_sum / cover[:, None] - centre[:, group_index * group_width:(group_index + 1) * group_width])
    return jnp.stack(pooled_parts, axis=1).astype(jnp.bfloat16)

def reference(mixer_input, mixer_gain, group_weight, mixer_scale, expert_input, expert_gain, routes, route_weight, w_gate, w_up, w_down):
    normed = normalize(mixer_input, mixer_gain)
    padded = jnp.pad(normed.astype(jnp.float32), ((8, 8), (0, 0)))
    pooled = pool_groups(padded, 0, TOKENS, TOKENS)
    mixed_groups = jnp.einsum('tgi,gio->tgo', pooled.astype(jnp.float32), group_weight.astype(jnp.float32))
    mixer_out = (mixed_groups.reshape(TOKENS, D) * mixer_scale).astype(jnp.bfloat16)
    expert_normed = normalize(expert_input, expert_gain)
    flat_route = routes.reshape(-1).astype(jnp.int32)
    flat_weight = route_weight.reshape(-1)
    most_rows = DEVICES * CAP
    block_width = FFE // N_TP

    def one_expert(running_out, inputs):
        gate_w, up_w, down_w, expert_index = inputs
        matches = flat_route == expert_index
        chosen = jnp.nonzero(matches, size=most_rows, fill_value=0)[0].astype(jnp.int32)
        live_rows = (jnp.arange(most_rows, dtype=jnp.int32) < jnp.sum(matches.astype(jnp.int32))).astype(jnp.float32)
        token_index = chosen // TOPK
        row_values = jnp.take(expert_normed, token_index, axis=0)
        gate_part = jnp.dot(row_values, gate_w, preferred_element_type=jnp.float32)
        up_part = jnp.dot(row_values, up_w, preferred_element_type=jnp.float32)
        hidden = (jax.nn.silu(gate_part) * up_part).astype(jnp.bfloat16)
        hidden_blocks = jnp.transpose(hidden.reshape(most_rows, N_TP, block_width), (1, 0, 2))
        weight_blocks = down_w.reshape(N_TP, block_width, D)

        def add_block(running, block_pair):
            hidden_block, weight_block = block_pair
            block_partial = lax.optimization_barrier(jnp.dot(hidden_block, weight_block, preferred_element_type=jnp.float32).astype(jnp.bfloat16))
            return (running + block_partial.astype(jnp.float32), None)
        summed, _ = lax.scan(add_block, jnp.zeros((most_rows, D), jnp.float32), (hidden_blocks, weight_blocks))
        expert_result = lax.optimization_barrier(summed.astype(jnp.bfloat16)).astype(jnp.float32)
        weights_here = jnp.take(flat_weight, chosen) * live_rows
        return (running_out.at[token_index].add(weights_here[:, None] * expert_result), None)
    total_out, _ = lax.scan(one_expert, jnp.zeros((TOKENS, D), jnp.float32), (w_gate, w_up, w_down, jnp.arange(EXPERTS, dtype=jnp.int32)))
    return (mixer_out, total_out.astype(jnp.bfloat16))
```

```python
import functools

import jax
import jax.numpy as jnp
from jax import lax
from jax.experimental import pallas as pl
from jax.experimental.pallas import tpu as pltpu
from jax.sharding import PartitionSpec as P

epsilon = 1e-06
vmem_share = 2**24


def padded_2(value, sides, width):
    for axis, dim in sides:
        size, length = (lax.axis_size(axis), value.shape[dim])
        up = [(i, (i + 1) % size) for i in range(size - 1)]
        down = [(j, i) for i, j in up]
        last = lax.slice_in_dim(value, length - width, length, axis=dim)
        leading = lax.slice_in_dim(value, 0, width, axis=dim)
        before = lax.ppermute(last, axis, up)
        after = lax.ppermute(leading, axis, down)
        value = jnp.concatenate([before, value, after], axis=dim)
    return value


def normalize(row_values, gain):
    values = row_values.astype(jnp.float32)
    scaled = values * lax.rsqrt(jnp.mean(values * values, axis=-1, keepdims=True) + epsilon)
    return (scaled * gain).astype(jnp.bfloat16)


def pool_groups(padded, start_row, row_count, seq_length):
    group_width = padded.shape[1] // 4
    position = start_row + jnp.arange(row_count, dtype=jnp.int32)
    centre = padded[8 : 8 + row_count]
    pooled_parts = []
    for group_index in range(4):
        window = 2 ** (group_index + 1)
        reach_left = window // 2
        reach_right = window - 1 - reach_left
        group_cols = padded[:, group_index * group_width : (group_index + 1) * group_width]
        window_sum = group_cols[8 - reach_left : 8 - reach_left + row_count]
        for offset in range(1 - reach_left, reach_right + 1):
            window_sum = window_sum + group_cols[8 + offset : 8 + offset + row_count]
        cover = (
            jnp.minimum(position + reach_right + 1, seq_length)
            - jnp.maximum(position - reach_left, 0)
        ).astype(jnp.float32)
        pooled_parts.append(
            window_sum / cover[:, None]
            - centre[:, group_index * group_width : (group_index + 1) * group_width]
        )
    return jnp.stack(pooled_parts, axis=1).astype(jnp.bfloat16)


def mixer(mixer_input, mixer_gain, group_weight, mixer_scale):
    row_count = mixer_input.shape[0]
    normed = normalize(mixer_input, mixer_gain)
    padded = padded_2(normed, ((("ep", "tp"), 0),), 8)
    start_row = lax.axis_index(("ep", "tp")) * row_count
    seq_length = row_count * lax.axis_size(("ep", "tp"))
    pooled = pool_groups(padded.astype(jnp.float32), start_row, row_count, seq_length)
    mixed_groups = jnp.einsum(
        "tgi,gio->tgo", pooled, group_weight, preferred_element_type=jnp.float32
    )
    return (mixed_groups.reshape(row_count, -1) * mixer_scale).astype(jnp.bfloat16)


def routed_plan(expert_input, expert_gain, routes, route_weight, w_gate, w_up, w_down):
    row_count = expert_input.shape[0]
    top_count = routes.shape[1]
    experts = lax.axis_size("ep") * w_gate.shape[0]
    capacity = 3 * top_count * row_count // (2 * experts)
    normed = normalize(expert_input, expert_gain)
    flat_route = routes.reshape(-1)
    onehot = (flat_route[:, None] == jnp.arange(experts, dtype=jnp.int32)[None, :]).astype(
        jnp.int32
    )
    before = jnp.cumsum(onehot, axis=0) - onehot
    slot_index = flat_route * capacity + jnp.sum(before * onehot, axis=1)
    places = (
        slot_index.reshape(row_count, top_count)[None, :, :]
        == jnp.arange(experts * capacity, dtype=jnp.int32)[:, None, None]
    )
    dispatch = jnp.any(places, axis=2).astype(jnp.bfloat16)
    outgoing = jnp.dot(dispatch, normed, preferred_element_type=jnp.float32).astype(jnp.bfloat16)
    arrived = lax.all_to_all(outgoing, "ep", split_axis=0, concat_axis=0, tiled=True)
    down_w = w_down[0]
    paired = jnp.stack((w_gate[0], w_up[0]), axis=0)
    portion = lax.all_gather(paired, "tp", axis=2, tiled=True)
    gate_part = jnp.dot(arrived, portion[0], preferred_element_type=jnp.float32)
    up_part = jnp.dot(arrived, portion[1], preferred_element_type=jnp.float32)
    hidden = (jax.nn.silu(gate_part) * up_part).astype(jnp.bfloat16)
    block_width = down_w.shape[0]
    portion = lax.all_gather(down_w, "tp", axis=0, tiled=True)
    blocks = portion.shape[0] // block_width
    hidden_part = hidden
    hidden_part = hidden_part.reshape(hidden_part.shape[0], blocks, block_width)
    block_terms = jnp.einsum(
        "rkf,kfd->krd",
        hidden_part,
        portion.reshape(blocks, block_width, portion.shape[1]),
        preferred_element_type=jnp.float32,
    )
    rounded = lax.optimization_barrier(block_terms.astype(jnp.bfloat16)).astype(jnp.float32)
    result = jnp.sum(rounded, axis=0)
    returned = lax.all_to_all(
        result.astype(jnp.bfloat16), "ep", split_axis=0, concat_axis=0, tiled=True
    )
    picked = (
        jnp.take(returned, slot_index, axis=0).astype(jnp.float32).reshape(row_count, top_count, -1)
    )
    expert_out = jnp.sum(picked * route_weight[:, :, None], axis=1).astype(jnp.bfloat16)
    return expert_out


def slots(routes, route_weight, experts):
    chosen = routes[:, :, None] == jnp.arange(experts, dtype=jnp.int32)[None, None, :]
    named = jnp.any(chosen, axis=1)
    weight = jnp.sum(jnp.where(chosen, route_weight[:, :, None], 0.0), axis=1)
    rows = routes.shape[0]
    earlier = jnp.arange(rows)[None, :] < jnp.arange(rows)[:, None]
    place = jnp.dot(
        earlier.astype(jnp.bfloat16), named.astype(jnp.bfloat16), preferred_element_type=jnp.float32
    )
    place = jnp.where(named, place, -1.0)
    return jnp.stack([place.T, weight.T], axis=1)


def near_first(length):
    return [sorted(range(length), key=lambda other: abs(other - at)) for at in range(length)]


def stream_kernel(
    depth, capacity,
    token_ref, listed_ref, gate_ref, up_ref, down_ref, out_ref,
    tok, res, from_core, half_low, half_high, from_right, from_left, from_above, from_below,
    send_sem, recv_sem, local_sem,
):
    column, line = lax.axis_index("ep"), lax.axis_index("tp")
    level, core = line // 2, line % 2
    other = 1 - core
    rows = token_ref.shape[0]
    half = rows // 2
    right_column, left_column = (2 * column + 1) % 5, (3 * column + 2) % 5
    right, left = (right_column, line), (left_column, line)
    beside = (column, level * 2 + other)
    above, below = (column, line + 2), (column, line - 2)
    has_above, has_below = level < depth - 1, level > 0

    def level_of(step):
        value = 0
        for at, order in enumerate(near_first(depth)):
            for turn, there in enumerate(order):
                value = value + there * jnp.where((level == at) & (step == turn), 1, 0)
        return value

    def link(src, dst, kind, at, target):
        return pltpu.make_async_remote_copy(
            src_ref=src, dst_ref=dst, send_sem=send_sem.at[kind, at],
            recv_sem=recv_sem.at[kind, at], device_id=target,
            device_id_type=pl.DeviceIdType.MESH,
        )

    def up(at):
        return link(tok.at[at, 0, core], tok.at[at, 0, core], 0, at, above)

    def down(at):
        return link(tok.at[at, 0, core], tok.at[at, 0, core], 1, at, below)

    def to_right(at):
        return link(tok.at[at, 0, core], tok.at[at, 1, core], 2, at, right)

    def to_left(at):
        return link(tok.at[at, 0, core], tok.at[at, 2, core], 3, at, left)

    def on_right(at):
        part = pl.ds(0, half)
        return link(tok.at[at, 1, core, part], tok.at[at, 3, core, part], 4, at, right)

    def on_left(at):
        part = pl.ds(half, half)
        return link(tok.at[at, 2, core, part], tok.at[at, 3, core, part], 5, at, left)

    def share(at, q):
        return link(tok.at[at, q, core], tok.at[at, q, core], 6 + q, at, beside)

    def shared_in(at, q):
        return link(tok.at[at, q, other], tok.at[at, q, other], 6 + q, at, beside)

    def give(at, q):
        return link(res.at[at, q, other], from_core.at[at, q], 10 + q, at, beside)

    def back_low(at):
        return link(res.at[at, 3, core, pl.ds(0, half)], half_low.at[at], 14, at, left)

    def back_high(at):
        return link(res.at[at, 3, core, pl.ds(half, half)], half_high.at[at], 15, at, right)

    def back_left(at):
        return link(res.at[at, 1, core], from_right.at[at], 16, at, left)

    def back_right(at):
        return link(res.at[at, 2, core], from_left.at[at], 17, at, right)

    def back_down(at):
        return link(res.at[at, 0, core], from_above.at[at], 18, at, below)

    def back_up(at):
        return link(res.at[at, 0, core], from_below.at[at], 19, at, above)

    barrier = pltpu.get_barrier_semaphore()

    def greet(target):
        pl.semaphore_signal(
            barrier, inc=1, device_id=target, device_id_type=pl.DeviceIdType.MESH
        )

    greet(right)
    greet(left)
    greet(beside)
    pl.when(has_above)(lambda: greet(above))
    pl.when(has_below)(lambda: greet(below))
    own_copy = pltpu.make_async_copy(token_ref, tok.at[level, 0, core], local_sem)
    own_copy.start()
    own_copy.wait()
    pl.semaphore_wait(barrier, 3 + jnp.where(has_above, 1, 0) + jnp.where(has_below, 1, 0))

    def compute(at, q):
        source = (
            jnp.where(q == 0, column, 0)
            + jnp.where(q == 1, left_column, 0)
            + jnp.where(q == 2, right_column, 0)
            + jnp.where(q == 3, 3 - column, 0)
        )
        picks, scales, chosen = [], [], []
        for lane in range(2):
            listed = listed_ref[source * (2 * depth) + at * 2 + lane]
            index = lax.broadcasted_iota(jnp.int32, (capacity, rows), 0).astype(jnp.float32)
            hit = index == listed[0:1, :]
            scales.append(jnp.sum(jnp.where(hit, listed[1:2, :], 0.0), axis=1, keepdims=True))
            picks.append(jnp.where(hit, 1.0, 0.0).astype(jnp.bfloat16))
            chosen.append(
                jnp.dot(picks[lane], tok[at, q, lane], preferred_element_type=jnp.float32)
                .astype(jnp.bfloat16)
            )
        gathered = jnp.concatenate(chosen, axis=0)
        gate_part = jnp.dot(gathered, gate_ref[...], preferred_element_type=jnp.float32)
        up_part = jnp.dot(gathered, up_ref[...], preferred_element_type=jnp.float32)
        hidden = (gate_part / (1.0 + jnp.exp(-gate_part)) * up_part).astype(jnp.bfloat16)
        partial = jnp.dot(hidden, down_ref[...], preferred_element_type=jnp.float32)
        partial = (partial * jnp.concatenate(scales, axis=0)).astype(jnp.bfloat16)
        for lane in range(2):
            res[at, q, lane] = lax.dot_general(
                picks[lane], partial[lane * capacity : (lane + 1) * capacity],
                (((0,), (0,)), ((), ())), preferred_element_type=jnp.float32,
            ).astype(jnp.bfloat16)

    def stage(turn, carry):
        @pl.when(turn < depth)
        def _():
            at = level_of(turn)
            pl.when(at < level)(lambda: up(at).wait_recv())
            pl.when(at > level)(lambda: down(at).wait_recv())
            pl.when((at <= level) & has_above)(lambda: up(at).start())
            pl.when((at >= level) & has_below)(lambda: down(at).start())
            to_right(at).start()
            to_left(at).start()
            share(at, 0).start()

        @pl.when((turn >= 1) & (turn < depth + 1))
        def _():
            at = level_of(turn - 1)
            to_right(at).wait_recv()
            on_right(at).start()
            share(at, 1).start()
            to_left(at).wait_recv()
            on_left(at).start()
            share(at, 2).start()

        @pl.when(turn >= 2)
        def _():
            at = level_of(turn - 2)
            on_right(at).wait_recv()
            on_left(at).wait_recv()
            share(at, 3).start()

        def one(q, inner):
            step = turn - (q + 1) // 2

            @pl.when((step >= 0) & (step < depth))
            def _():
                at = level_of(step)
                shared_in(at, q).wait_recv()
                compute(at, q)
                give(at, q).start()

            return inner

        lax.fori_loop(0, 4, one, 0)
        return carry

    lax.fori_loop(0, depth + 2, stage, 0)

    piece = half // 3 if half % 48 == 0 else half
    f32 = jnp.float32

    def add(at, q, start, count, terms):
        def body(i, carry):
            span = pl.ds(pl.multiple_of(start + i * piece, piece), piece)
            there = pl.ds(pl.multiple_of(i * piece, piece), piece)
            total = res[at, q, core, span].astype(f32) + from_core[at, q, span].astype(f32)
            for term in terms:
                total = total + term[at, there].astype(f32)
            res[at, q, core, span] = total.astype(jnp.bfloat16)
            return carry

        lax.fori_loop(0, count // piece, body, 0)

    def extend(at, term):
        def body(i, carry):
            span = pl.ds(pl.multiple_of(i * piece, piece), piece)
            res[at, 0, core, span] = (
                res[at, 0, core, span].astype(f32) + term[at, span].astype(f32)
            ).astype(jnp.bfloat16)
            return carry

        lax.fori_loop(0, rows // piece, body, 0)

    def corner(turn, carry):
        at = level_of(depth - 1 - turn)
        give(at, 3).wait_recv()
        add(at, 3, 0, rows, [])
        back_low(at).start()
        back_high(at).start()
        return carry

    def sides(at):
        give(at, 1).wait_recv()
        back_low(at).wait_recv()
        add(at, 1, 0, half, [half_low])
        add(at, 1, half, half, [])
        back_left(at).start()
        give(at, 2).wait_recv()
        back_high(at).wait_recv()
        add(at, 2, 0, half, [])
        add(at, 2, half, half, [half_high])
        back_right(at).start()

    def home(at):
        give(at, 0).wait_recv()
        back_left(at).wait_recv()
        back_right(at).wait_recv()
        add(at, 0, 0, rows, [from_right, from_left])

        @pl.when((at <= level) & has_above)
        def _():
            back_down(at).wait_recv()
            extend(at, from_above)

        @pl.when((at >= level) & has_below)
        def _():
            back_up(at).wait_recv()
            extend(at, from_below)

        pl.when(at < level)(lambda: back_down(at).start())
        pl.when(at > level)(lambda: back_up(at).start())

    def finish(turn, carry):
        pl.when(turn < depth)(lambda: sides(level_of(depth - 1 - turn)))
        pl.when(turn >= 1)(lambda: home(level_of(depth - turn)))
        return carry

    lax.fori_loop(0, depth, corner, 0)
    lax.fori_loop(0, depth + 1, finish, 0)
    out_copy = pltpu.make_async_copy(res.at[level, 0, core], out_ref, local_sem)
    out_copy.start()

    def drain(at, carry):
        pl.when((at <= level) & has_above)(lambda: up(at).wait_send())
        pl.when((at >= level) & has_below)(lambda: down(at).wait_send())
        for copy in (to_right, to_left, on_right, on_left):
            copy(at).wait_send()
        for copy in (back_low, back_high, back_left, back_right):
            copy(at).wait_send()
        for q in range(4):
            share(at, q).wait_send()
            give(at, q).wait_send()
        pl.when(at < level)(lambda: back_down(at).wait_send())
        pl.when(at > level)(lambda: back_up(at).wait_send())
        return carry

    lax.fori_loop(0, depth, drain, 0)
    out_copy.wait()


def dense_plan(expert_input, expert_gain, routes, route_weight, w_gate, w_up, w_down):
    row_count, width = expert_input.shape
    experts = lax.axis_size("ep")
    depth = lax.axis_size("tp") // 2
    capacity = 3 * routes.shape[1] * row_count // (2 * experts)
    axes = ("ep", "tp")
    normed = normalize(expert_input, expert_gain)
    listed = lax.all_gather(slots(routes, route_weight, experts), axes, axis=0)
    mine = lax.dynamic_index_in_dim(listed, lax.axis_index("ep"), axis=1, keepdims=False)
    bf16 = jnp.bfloat16
    half = row_count // 2
    vmem = pl.BlockSpec(memory_space=pltpu.VMEM)
    return pl.pallas_call(
        functools.partial(stream_kernel, depth, capacity),
        out_shape=jax.ShapeDtypeStruct((row_count, width), bf16),
        in_specs=[vmem] * 5,
        out_specs=vmem,
        scratch_shapes=[
            pltpu.VMEM((depth, 4, 2, row_count, width), bf16),
            pltpu.VMEM((depth, 4, 2, row_count, width), bf16),
            pltpu.VMEM((depth, 4, row_count, width), bf16),
            pltpu.VMEM((depth, half, width), bf16),
            pltpu.VMEM((depth, half, width), bf16),
            pltpu.VMEM((depth, row_count, width), bf16),
            pltpu.VMEM((depth, row_count, width), bf16),
            pltpu.VMEM((depth, row_count, width), bf16),
            pltpu.VMEM((depth, row_count, width), bf16),
            pltpu.SemaphoreType.DMA((20, depth)),
            pltpu.SemaphoreType.DMA((20, depth)),
            pltpu.SemaphoreType.DMA,
        ],
        compiler_params=pltpu.CompilerParams(
            collective_id=0, has_side_effects=True, vmem_limit_bytes=60 * 2**20
        ),
    )(normed, mine, w_gate[0], w_up[0], w_down[0])


def on_device(
    mixer_input, mixer_gain, group_weight, mixer_scale,
    expert_input, expert_gain, routes, route_weight, w_gate, w_up, w_down,
):
    devices = lax.axis_size(("ep", "tp"))
    gathered_bytes = 2 * devices * expert_input.size
    square = lax.axis_size("ep") == 4
    plan = dense_plan if square and gathered_bytes <= vmem_share else routed_plan
    expert_out = plan(expert_input, expert_gain, routes, route_weight, w_gate, w_up, w_down)
    return (mixer(mixer_input, mixer_gain, group_weight, mixer_scale), expert_out)


def solution(mesh):
    placed = (
        P(("ep", "tp"), None),
        P(),
        P(),
        P(),
        P(("ep", "tp"), None),
        P(),
        P(("ep", "tp"), None),
        P(("ep", "tp"), None),
        P("ep", None, "tp"),
        P("ep", None, "tp"),
        P("ep", "tp", None),
    )
    return jax.shard_map(
        on_device,
        mesh=mesh,
        in_specs=placed,
        out_specs=(P(("ep", "tp"), None), P(("ep", "tp"), None)),
        check_vma=False,
    )
```

```python
import functools

import jax
import jax.numpy as jnp
from jax import lax
from jax.experimental import pallas as pl
from jax.experimental.pallas import tpu as pltpu
from jax.sharding import PartitionSpec as P

epsilon = 1e-06
vmem_share = 2**24


def padded_2(value, sides, width):
    for axis, dim in sides:
        size, length = (lax.axis_size(axis), value.shape[dim])
        up = [(i, (i + 1) % size) for i in range(size - 1)]
        down = [(j, i) for i, j in up]
        last = lax.slice_in_dim(value, length - width, length, axis=dim)
        leading = lax.slice_in_dim(value, 0, width, axis=dim)
        before = lax.ppermute(last, axis, up)
        after = lax.ppermute(leading, axis, down)
        value = jnp.concatenate([before, value, after], axis=dim)
    return value


def normalize(row_values, gain):
    values = row_values.astype(jnp.float32)
    scaled = values * lax.rsqrt(jnp.mean(values * values, axis=-1, keepdims=True) + epsilon)
    return (scaled * gain).astype(jnp.bfloat16)


def pool_groups(padded, start_row, row_count, seq_length):
    group_width = padded.shape[1] // 4
    position = start_row + jnp.arange(row_count, dtype=jnp.int32)
    centre = padded[8 : 8 + row_count]
    pooled_parts = []
    for group_index in range(4):
        window = 2 ** (group_index + 1)
        reach_left = window // 2
        reach_right = window - 1 - reach_left
        group_cols = padded[:, group_index * group_width : (group_index + 1) * group_width]
        window_sum = group_cols[8 - reach_left : 8 - reach_left + row_count]
        for offset in range(1 - reach_left, reach_right + 1):
            window_sum = window_sum + group_cols[8 + offset : 8 + offset + row_count]
        cover = (
            jnp.minimum(position + reach_right + 1, seq_length)
            - jnp.maximum(position - reach_left, 0)
        ).astype(jnp.float32)
        pooled_parts.append(
            window_sum / cover[:, None]
            - centre[:, group_index * group_width : (group_index + 1) * group_width]
        )
    return jnp.stack(pooled_parts, axis=1).astype(jnp.bfloat16)


def mixer(mixer_input, mixer_gain, group_weight, mixer_scale):
    row_count = mixer_input.shape[0]
    normed = normalize(mixer_input, mixer_gain)
    padded = padded_2(normed, ((("ep", "tp"), 0),), 8)
    start_row = lax.axis_index(("ep", "tp")) * row_count
    seq_length = row_count * lax.axis_size(("ep", "tp"))
    pooled = pool_groups(padded.astype(jnp.float32), start_row, row_count, seq_length)
    mixed_groups = jnp.einsum(
        "tgi,gio->tgo", pooled, group_weight, preferred_element_type=jnp.float32
    )
    return (mixed_groups.reshape(row_count, -1) * mixer_scale).astype(jnp.bfloat16)


def routed_plan(expert_input, expert_gain, routes, route_weight, w_gate, w_up, w_down):
    row_count = expert_input.shape[0]
    top_count = routes.shape[1]
    experts = lax.axis_size("ep") * w_gate.shape[0]
    capacity = 3 * top_count * row_count // (2 * experts)
    normed = normalize(expert_input, expert_gain)
    flat_route = routes.reshape(-1)
    onehot = (flat_route[:, None] == jnp.arange(experts, dtype=jnp.int32)[None, :]).astype(
        jnp.int32
    )
    before = jnp.cumsum(onehot, axis=0) - onehot
    slot_index = flat_route * capacity + jnp.sum(before * onehot, axis=1)
    places = (
        slot_index.reshape(row_count, top_count)[None, :, :]
        == jnp.arange(experts * capacity, dtype=jnp.int32)[:, None, None]
    )
    dispatch = jnp.any(places, axis=2).astype(jnp.bfloat16)
    outgoing = jnp.dot(dispatch, normed, preferred_element_type=jnp.float32).astype(jnp.bfloat16)
    arrived = lax.all_to_all(outgoing, "ep", split_axis=0, concat_axis=0, tiled=True)
    down_w = w_down[0]
    paired = jnp.stack((w_gate[0], w_up[0]), axis=0)
    portion = lax.all_gather(paired, "tp", axis=2, tiled=True)
    gate_part = jnp.dot(arrived, portion[0], preferred_element_type=jnp.float32)
    up_part = jnp.dot(arrived, portion[1], preferred_element_type=jnp.float32)
    hidden = (jax.nn.silu(gate_part) * up_part).astype(jnp.bfloat16)
    block_width = down_w.shape[0]
    portion = lax.all_gather(down_w, "tp", axis=0, tiled=True)
    blocks = portion.shape[0] // block_width
    hidden_part = hidden
    hidden_part = hidden_part.reshape(hidden_part.shape[0], blocks, block_width)
    block_terms = jnp.einsum(
        "rkf,kfd->krd",
        hidden_part,
        portion.reshape(blocks, block_width, portion.shape[1]),
        preferred_element_type=jnp.float32,
    )
    rounded = lax.optimization_barrier(block_terms.astype(jnp.bfloat16)).astype(jnp.float32)
    result = jnp.sum(rounded, axis=0)
    returned = lax.all_to_all(
        result.astype(jnp.bfloat16), "ep", split_axis=0, concat_axis=0, tiled=True
    )
    picked = (
        jnp.take(returned, slot_index, axis=0).astype(jnp.float32).reshape(row_count, top_count, -1)
    )
    expert_out = jnp.sum(picked * route_weight[:, :, None], axis=1).astype(jnp.bfloat16)
    return expert_out


def slots(routes, route_weight, experts):
    chosen = routes[:, :, None] == jnp.arange(experts, dtype=jnp.int32)[None, None, :]
    named = jnp.any(chosen, axis=1)
    weight = jnp.sum(jnp.where(chosen, route_weight[:, :, None], 0.0), axis=1)
    rows = routes.shape[0]
    earlier = jnp.arange(rows)[None, :] < jnp.arange(rows)[:, None]
    place = jnp.dot(
        earlier.astype(jnp.bfloat16), named.astype(jnp.bfloat16), preferred_element_type=jnp.float32
    )
    place = jnp.where(named, place, -1.0)
    high = lax.reduce_precision(weight, 8, 7)
    return jnp.concatenate([place, high, weight - high], axis=1).T.astype(jnp.bfloat16)


def near_first(length):
    return [sorted(range(length), key=lambda other: abs(other - at)) for at in range(length)]


def stream_kernel(
    depth, capacity, experts,
    token_ref, gate_ref, up_ref, down_ref, out_ref,
    tok, res, from_core, half_low, half_high, from_right, from_left, from_above, from_below,
    send_sem, recv_sem, local_sem,
):
    column, line = lax.axis_index("ep"), lax.axis_index("tp")
    level, core = line // 2, line % 2
    other = 1 - core
    tall = token_ref.shape[0]
    rows = out_ref.shape[0]
    half = rows // 2
    right_column, left_column = (2 * column + 1) % 5, (3 * column + 2) % 5
    right, left = (right_column, line), (left_column, line)
    beside = (column, level * 2 + other)
    above, below = (column, line + 2), (column, line - 2)
    has_above, has_below = level < depth - 1, level > 0

    def level_of(step):
        value = 0
        for at, order in enumerate(near_first(depth)):
            for turn, there in enumerate(order):
                value = value + there * jnp.where((level == at) & (step == turn), 1, 0)
        return value

    def link(src, dst, kind, at, target):
        return pltpu.make_async_remote_copy(
            src_ref=src, dst_ref=dst, send_sem=send_sem.at[kind, at],
            recv_sem=recv_sem.at[kind, at], device_id=target,
            device_id_type=pl.DeviceIdType.MESH,
        )

    def up(at):
        return link(tok.at[at, 0, core], tok.at[at, 0, core], 0, at, above)

    def down(at):
        return link(tok.at[at, 0, core], tok.at[at, 0, core], 1, at, below)

    def to_right(at):
        return link(tok.at[at, 0, core], tok.at[at, 1, core], 2, at, right)

    def to_left(at):
        return link(tok.at[at, 0, core], tok.at[at, 2, core], 3, at, left)

    def on_right(at):
        part = pl.ds(0, half)
        return link(tok.at[at, 1, core, part], tok.at[at, 3, core, part], 4, at, right)

    def on_left(at):
        part = pl.ds(half, tall - half)
        return link(tok.at[at, 2, core, part], tok.at[at, 3, core, part], 5, at, left)

    def share(at, q):
        return link(tok.at[at, q, core], tok.at[at, q, core], 6 + q, at, beside)

    def shared_in(at, q):
        return link(tok.at[at, q, other], tok.at[at, q, other], 6 + q, at, beside)

    def give(at, q):
        return link(res.at[at, q, other], from_core.at[at, q], 10 + q, at, beside)

    def back_low(at):
        return link(res.at[at, 3, core, pl.ds(0, half)], half_low.at[at], 14, at, left)

    def back_high(at):
        return link(res.at[at, 3, core, pl.ds(half, half)], half_high.at[at], 15, at, right)

    def back_left(at):
        return link(res.at[at, 1, core], from_right.at[at], 16, at, left)

    def back_right(at):
        return link(res.at[at, 2, core], from_left.at[at], 17, at, right)

    def back_down(at):
        return link(res.at[at, 0, core], from_above.at[at], 18, at, below)

    def back_up(at):
        return link(res.at[at, 0, core], from_below.at[at], 19, at, above)

    barrier = pltpu.get_barrier_semaphore()

    def greet(target):
        pl.semaphore_signal(
            barrier, inc=1, device_id=target, device_id_type=pl.DeviceIdType.MESH
        )

    greet(right)
    greet(left)
    greet(beside)
    pl.when(has_above)(lambda: greet(above))
    pl.when(has_below)(lambda: greet(below))
    own_copy = pltpu.make_async_copy(token_ref, tok.at[level, 0, core], local_sem)
    own_copy.start()
    own_copy.wait()
    pl.semaphore_wait(barrier, 3 + jnp.where(has_above, 1, 0) + jnp.where(has_below, 1, 0))

    piece = half // 3 if half % 48 == 0 else half
    f32 = jnp.float32

    def add(at, q, start, count, terms):
        def body(i, carry):
            span = pl.ds(pl.multiple_of(start + i * piece, piece), piece)
            there = pl.ds(pl.multiple_of(i * piece, piece), piece)
            total = res[at, q, core, span].astype(f32) + from_core[at, q, span].astype(f32)
            for term in terms:
                total = total + term[at, there].astype(f32)
            res[at, q, core, span] = total.astype(jnp.bfloat16)
            return carry

        lax.fori_loop(0, count // piece, body, 0)

    def corner(at):
        give(at, 3).wait_recv()
        add(at, 3, 0, rows, [])
        back_low(at).start()
        back_high(at).start()

    def compute(at, q):
        picks, scales, chosen = [], [], []
        for lane in range(2):
            listed = tok[at, q, lane, pl.ds(rows, tall - rows), pl.ds(0, rows)].astype(f32)
            listing = lax.broadcasted_iota(jnp.int32, listed.shape, 0)

            def row_of(index):
                return jnp.sum(jnp.where(listing == index, listed, 0.0), axis=0, keepdims=True)

            weight = row_of(experts + column) + row_of(2 * experts + column)
            index = lax.broadcasted_iota(jnp.int32, (capacity, rows), 0).astype(jnp.float32)
            hit = index == row_of(column)
            scales.append(jnp.sum(jnp.where(hit, weight, 0.0), axis=1, keepdims=True))
            picks.append(jnp.where(hit, 1.0, 0.0).astype(jnp.bfloat16))
            chosen.append(
                jnp.dot(picks[lane], tok[at, q, lane, pl.ds(0, rows)], preferred_element_type=jnp.float32)
                .astype(jnp.bfloat16)
            )
        gathered = jnp.concatenate(chosen, axis=0)
        gate_part = jnp.dot(gathered, gate_ref[...], preferred_element_type=jnp.float32)
        up_part = jnp.dot(gathered, up_ref[...], preferred_element_type=jnp.float32)
        hidden = (gate_part / (1.0 + jnp.exp(-gate_part)) * up_part).astype(jnp.bfloat16)
        partial = jnp.dot(hidden, down_ref[...], preferred_element_type=jnp.float32)
        partial = (partial * jnp.concatenate(scales, axis=0)).astype(jnp.bfloat16)
        for lane in range(2):
            res[at, q, lane] = lax.dot_general(
                picks[lane], partial[lane * capacity : (lane + 1) * capacity],
                (((0,), (0,)), ((), ())), preferred_element_type=jnp.float32,
            ).astype(jnp.bfloat16)

    def stage(turn, carry):
        @pl.when(turn < depth)
        def _():
            at = level_of(turn)
            pl.when(at < level)(lambda: up(at).wait_recv())
            pl.when(at > level)(lambda: down(at).wait_recv())
            pl.when((at <= level) & has_above)(lambda: up(at).start())
            pl.when((at >= level) & has_below)(lambda: down(at).start())
            to_right(at).start()
            to_left(at).start()
            share(at, 0).start()

        @pl.when((turn >= 1) & (turn < depth + 1))
        def _():
            at = level_of(turn - 1)
            to_right(at).wait_recv()
            on_right(at).start()
            share(at, 1).start()
            to_left(at).wait_recv()
            on_left(at).start()
            share(at, 2).start()

        @pl.when((turn >= 2) & (turn < depth + 2))
        def _():
            at = level_of(turn - 2)
            on_right(at).wait_recv()
            on_left(at).wait_recv()
            share(at, 3).start()

        pl.when(turn >= 3)(lambda: corner(level_of(turn - 3)))

        def one(q, inner):
            step = turn - (q + 1) // 2

            @pl.when((step >= 0) & (step < depth))
            def _():
                at = level_of(step)
                shared_in(at, q).wait_recv()
                compute(at, q)
                give(at, q).start()

            return inner

        lax.fori_loop(0, 4, one, 0)
        return carry

    lax.fori_loop(0, depth + 3, stage, 0)

    def extend(at, term):
        def body(i, carry):
            span = pl.ds(pl.multiple_of(i * piece, piece), piece)
            res[at, 0, core, span] = (
                res[at, 0, core, span].astype(f32) + term[at, span].astype(f32)
            ).astype(jnp.bfloat16)
            return carry

        lax.fori_loop(0, rows // piece, body, 0)

    def sides(at):
        give(at, 1).wait_recv()
        back_low(at).wait_recv()
        add(at, 1, 0, half, [half_low])
        add(at, 1, half, half, [])
        back_left(at).start()
        give(at, 2).wait_recv()
        back_high(at).wait_recv()
        add(at, 2, 0, half, [])
        add(at, 2, half, half, [half_high])
        back_right(at).start()

    def home(at):
        give(at, 0).wait_recv()
        back_left(at).wait_recv()
        back_right(at).wait_recv()
        add(at, 0, 0, rows, [from_right, from_left])

        @pl.when((at <= level) & has_above)
        def _():
            back_down(at).wait_recv()
            extend(at, from_above)

        @pl.when((at >= level) & has_below)
        def _():
            back_up(at).wait_recv()
            extend(at, from_below)

        pl.when(at < level)(lambda: back_down(at).start())
        pl.when(at > level)(lambda: back_up(at).start())

    def finish(turn, carry):
        pl.when(turn < depth)(lambda: sides(level_of(depth - 1 - turn)))
        pl.when(turn >= 1)(lambda: home(level_of(depth - turn)))
        return carry

    lax.fori_loop(0, depth + 1, finish, 0)
    out_copy = pltpu.make_async_copy(res.at[level, 0, core], out_ref, local_sem)
    out_copy.start()

    def drain(at, carry):
        pl.when((at <= level) & has_above)(lambda: up(at).wait_send())
        pl.when((at >= level) & has_below)(lambda: down(at).wait_send())
        for copy in (to_right, to_left, on_right, on_left):
            copy(at).wait_send()
        for copy in (back_low, back_high, back_left, back_right):
            copy(at).wait_send()
        for q in range(4):
            share(at, q).wait_send()
            give(at, q).wait_send()
        pl.when(at < level)(lambda: back_down(at).wait_send())
        pl.when(at > level)(lambda: back_up(at).wait_send())
        return carry

    lax.fori_loop(0, depth, drain, 0)
    out_copy.wait()


def dense_plan(expert_input, expert_gain, routes, route_weight, w_gate, w_up, w_down):
    row_count, width = expert_input.shape
    experts = lax.axis_size("ep")
    depth = lax.axis_size("tp") // 2
    capacity = 3 * routes.shape[1] * row_count // (2 * experts)
    normed = normalize(expert_input, expert_gain)
    listed = slots(routes, route_weight, experts)
    pad = -(-3 * experts // 16) * 16
    listed = jnp.pad(listed, ((0, pad - 3 * experts), (0, width - row_count)))
    sent = jnp.concatenate([normed, listed], axis=0)
    bf16 = jnp.bfloat16
    half = row_count // 2
    vmem = pl.BlockSpec(memory_space=pltpu.VMEM)
    return pl.pallas_call(
        functools.partial(stream_kernel, depth, capacity, experts),
        out_shape=jax.ShapeDtypeStruct((row_count, width), bf16),
        in_specs=[vmem] * 4,
        out_specs=vmem,
        scratch_shapes=[
            pltpu.VMEM((depth, 4, 2, row_count + pad, width), bf16),
            pltpu.VMEM((depth, 4, 2, row_count, width), bf16),
            pltpu.VMEM((depth, 4, row_count, width), bf16),
            pltpu.VMEM((depth, half, width), bf16),
            pltpu.VMEM((depth, half, width), bf16),
            pltpu.VMEM((depth, row_count, width), bf16),
            pltpu.VMEM((depth, row_count, width), bf16),
            pltpu.VMEM((depth, row_count, width), bf16),
            pltpu.VMEM((depth, row_count, width), bf16),
            pltpu.SemaphoreType.DMA((20, depth)),
            pltpu.SemaphoreType.DMA((20, depth)),
            pltpu.SemaphoreType.DMA,
        ],
        compiler_params=pltpu.CompilerParams(
            collective_id=0, has_side_effects=True, vmem_limit_bytes=60 * 2**20
        ),
    )(sent, w_gate[0], w_up[0], w_down[0])


def on_device(
    mixer_input, mixer_gain, group_weight, mixer_scale,
    expert_input, expert_gain, routes, route_weight, w_gate, w_up, w_down,
):
    devices = lax.axis_size(("ep", "tp"))
    gathered_bytes = 2 * devices * expert_input.size
    square = lax.axis_size("ep") == 4
    plan = dense_plan if square and gathered_bytes <= vmem_share else routed_plan
    expert_out = plan(expert_input, expert_gain, routes, route_weight, w_gate, w_up, w_down)
    return (mixer(mixer_input, mixer_gain, group_weight, mixer_scale), expert_out)


def solution(mesh):
    placed = (
        P(("ep", "tp"), None),
        P(),
        P(),
        P(),
        P(("ep", "tp"), None),
        P(),
        P(("ep", "tp"), None),
        P(("ep", "tp"), None),
        P("ep", None, "tp"),
        P("ep", None, "tp"),
        P("ep", "tp", None),
    )
    return jax.shard_map(
        on_device,
        mesh=mesh,
        in_specs=placed,
        out_specs=(P(("ep", "tp"), None), P(("ep", "tp"), None)),
        check_vma=False,
    )
```

```python
import functools

import jax
import jax.numpy as jnp
from jax import lax
from jax.experimental import pallas as pl
from jax.experimental.pallas import tpu as pltpu
from jax.sharding import PartitionSpec as P

epsilon = 1e-06
vmem_share = 2**24


def padded_2(value, sides, width):
    for axis, dim in sides:
        size, length = (lax.axis_size(axis), value.shape[dim])
        up = [(i, (i + 1) % size) for i in range(size - 1)]
        down = [(j, i) for i, j in up]
        last = lax.slice_in_dim(value, length - width, length, axis=dim)
        leading = lax.slice_in_dim(value, 0, width, axis=dim)
        before = lax.ppermute(last, axis, up)
        after = lax.ppermute(leading, axis, down)
        value = jnp.concatenate([before, value, after], axis=dim)
    return value


def normalize(row_values, gain):
    values = row_values.astype(jnp.float32)
    scaled = values * lax.rsqrt(jnp.mean(values * values, axis=-1, keepdims=True) + epsilon)
    return (scaled * gain).astype(jnp.bfloat16)


def pool_groups(padded, start_row, row_count, seq_length):
    group_width = padded.shape[1] // 4
    position = start_row + jnp.arange(row_count, dtype=jnp.int32)
    centre = padded[8 : 8 + row_count]
    pooled_parts = []
    for group_index in range(4):
        window = 2 ** (group_index + 1)
        reach_left = window // 2
        reach_right = window - 1 - reach_left
        group_cols = padded[:, group_index * group_width : (group_index + 1) * group_width]
        window_sum = group_cols[8 - reach_left : 8 - reach_left + row_count]
        for offset in range(1 - reach_left, reach_right + 1):
            window_sum = window_sum + group_cols[8 + offset : 8 + offset + row_count]
        cover = (
            jnp.minimum(position + reach_right + 1, seq_length)
            - jnp.maximum(position - reach_left, 0)
        ).astype(jnp.float32)
        pooled_parts.append(
            window_sum / cover[:, None]
            - centre[:, group_index * group_width : (group_index + 1) * group_width]
        )
    return jnp.stack(pooled_parts, axis=1).astype(jnp.bfloat16)


def mixer(mixer_input, mixer_gain, group_weight, mixer_scale):
    row_count = mixer_input.shape[0]
    normed = normalize(mixer_input, mixer_gain)
    padded = padded_2(normed, ((("ep", "tp"), 0),), 8)
    start_row = lax.axis_index(("ep", "tp")) * row_count
    seq_length = row_count * lax.axis_size(("ep", "tp"))
    pooled = pool_groups(padded.astype(jnp.float32), start_row, row_count, seq_length)
    mixed_groups = jnp.einsum(
        "tgi,gio->tgo", pooled, group_weight, preferred_element_type=jnp.float32
    )
    return (mixed_groups.reshape(row_count, -1) * mixer_scale).astype(jnp.bfloat16)


def routed_plan(expert_input, expert_gain, routes, route_weight, w_gate, w_up, w_down):
    row_count = expert_input.shape[0]
    top_count = routes.shape[1]
    experts = lax.axis_size("ep") * w_gate.shape[0]
    capacity = 3 * top_count * row_count // (2 * experts)
    normed = normalize(expert_input, expert_gain)
    flat_route = routes.reshape(-1)
    onehot = (flat_route[:, None] == jnp.arange(experts, dtype=jnp.int32)[None, :]).astype(
        jnp.int32
    )
    before = jnp.cumsum(onehot, axis=0) - onehot
    slot_index = flat_route * capacity + jnp.sum(before * onehot, axis=1)
    places = (
        slot_index.reshape(row_count, top_count)[None, :, :]
        == jnp.arange(experts * capacity, dtype=jnp.int32)[:, None, None]
    )
    dispatch = jnp.any(places, axis=2).astype(jnp.bfloat16)
    outgoing = jnp.dot(dispatch, normed, preferred_element_type=jnp.float32).astype(jnp.bfloat16)
    arrived = lax.all_to_all(outgoing, "ep", split_axis=0, concat_axis=0, tiled=True)
    down_w = w_down[0]
    paired = jnp.stack((w_gate[0], w_up[0]), axis=0)
    portion = lax.all_gather(paired, "tp", axis=2, tiled=True)
    gate_part = jnp.dot(arrived, portion[0], preferred_element_type=jnp.float32)
    up_part = jnp.dot(arrived, portion[1], preferred_element_type=jnp.float32)
    hidden = (jax.nn.silu(gate_part) * up_part).astype(jnp.bfloat16)
    block_width = down_w.shape[0]
    portion = lax.all_gather(down_w, "tp", axis=0, tiled=True)
    blocks = portion.shape[0] // block_width
    hidden_part = hidden
    hidden_part = hidden_part.reshape(hidden_part.shape[0], blocks, block_width)
    block_terms = jnp.einsum(
        "rkf,kfd->krd",
        hidden_part,
        portion.reshape(blocks, block_width, portion.shape[1]),
        preferred_element_type=jnp.float32,
    )
    rounded = lax.optimization_barrier(block_terms.astype(jnp.bfloat16)).astype(jnp.float32)
    result = jnp.sum(rounded, axis=0)
    returned = lax.all_to_all(
        result.astype(jnp.bfloat16), "ep", split_axis=0, concat_axis=0, tiled=True
    )
    picked = (
        jnp.take(returned, slot_index, axis=0).astype(jnp.float32).reshape(row_count, top_count, -1)
    )
    expert_out = jnp.sum(picked * route_weight[:, :, None], axis=1).astype(jnp.bfloat16)
    return expert_out


def slots(routes, route_weight, experts):
    chosen = routes[:, :, None] == jnp.arange(experts, dtype=jnp.int32)[None, None, :]
    named = jnp.any(chosen, axis=1)
    weight = jnp.sum(jnp.where(chosen, route_weight[:, :, None], 0.0), axis=1)
    rows = routes.shape[0]
    earlier = jnp.arange(rows)[None, :] < jnp.arange(rows)[:, None]
    place = jnp.dot(
        earlier.astype(jnp.bfloat16), named.astype(jnp.bfloat16), preferred_element_type=jnp.float32
    )
    place = jnp.where(named, place, -1.0)
    high = lax.reduce_precision(weight, 8, 7)
    return jnp.concatenate([place, high, weight - high], axis=1).T.astype(jnp.bfloat16)


def near_first(length):
    return [sorted(range(length), key=lambda other: abs(other - at)) for at in range(length)]


def stream_kernel(
    depth, capacity, experts,
    token_ref, gate_ref, up_ref, down_ref, out_ref,
    tok, res, from_core, half_low, half_high, from_right, from_left, from_above, from_below,
    send_sem, recv_sem, local_sem,
):
    column, line = lax.axis_index("ep"), lax.axis_index("tp")
    level, core = line // 2, line % 2
    other = 1 - core
    tall = token_ref.shape[0]
    rows = out_ref.shape[0]
    half = rows // 2
    right_column, left_column = (2 * column + 1) % 5, (3 * column + 2) % 5
    right, left = (right_column, line), (left_column, line)
    beside = (column, level * 2 + other)
    above, below = (column, line + 2), (column, line - 2)
    has_above, has_below = level < depth - 1, level > 0

    def level_of(step):
        value = 0
        for at, order in enumerate(near_first(depth)):
            for turn, there in enumerate(order):
                value = value + there * jnp.where((level == at) & (step == turn), 1, 0)
        return value

    def link(src, dst, kind, at, target):
        return pltpu.make_async_remote_copy(
            src_ref=src, dst_ref=dst, send_sem=send_sem.at[kind, at],
            recv_sem=recv_sem.at[kind, at], device_id=target,
            device_id_type=pl.DeviceIdType.MESH,
        )

    def up(at):
        return link(tok.at[at, 0, core], tok.at[at, 0, core], 0, at, above)

    def down(at):
        return link(tok.at[at, 0, core], tok.at[at, 0, core], 1, at, below)

    def to_right(at):
        return link(tok.at[at, 0, core], tok.at[at, 1, core], 2, at, right)

    def to_left(at):
        return link(tok.at[at, 0, core], tok.at[at, 2, core], 3, at, left)

    def on_right(at):
        part = pl.ds(0, half)
        return link(tok.at[at, 1, core, part], tok.at[at, 3, core, part], 4, at, right)

    def on_left(at):
        part = pl.ds(half, tall - half)
        return link(tok.at[at, 2, core, part], tok.at[at, 3, core, part], 5, at, left)

    def share(at, q):
        return link(tok.at[at, q, core], tok.at[at, q, core], 6 + q, at, beside)

    def shared_in(at, q):
        return link(tok.at[at, q, other], tok.at[at, q, other], 6 + q, at, beside)

    def give(at, q):
        return link(res.at[at, q, other], from_core.at[at, q], 10 + q, at, beside)

    def back_low(at):
        return link(res.at[at, 3, core, pl.ds(0, half)], half_low.at[at], 14, at, left)

    def back_high(at):
        return link(res.at[at, 3, core, pl.ds(half, half)], half_high.at[at], 15, at, right)

    def back_left(at):
        return link(res.at[at, 1, core], from_right.at[at], 16, at, left)

    def back_right(at):
        return link(res.at[at, 2, core], from_left.at[at], 17, at, right)

    def back_down(at):
        return link(res.at[at, 0, core], from_above.at[at], 18, at, below)

    def back_up(at):
        return link(res.at[at, 0, core], from_below.at[at], 19, at, above)

    barrier = pltpu.get_barrier_semaphore()

    def greet(target):
        pl.semaphore_signal(
            barrier, inc=1, device_id=target, device_id_type=pl.DeviceIdType.MESH
        )

    greet(right)
    greet(left)
    greet(beside)
    pl.when(has_above)(lambda: greet(above))
    pl.when(has_below)(lambda: greet(below))
    own_copy = pltpu.make_async_copy(token_ref, tok.at[level, 0, core], local_sem)
    own_copy.start()
    own_copy.wait()
    pl.semaphore_wait(barrier, 3 + jnp.where(has_above, 1, 0) + jnp.where(has_below, 1, 0))

    piece = half // 3 if half % 48 == 0 else half
    f32 = jnp.float32

    def add(at, q, start, count, terms):
        def body(i, carry):
            span = pl.ds(pl.multiple_of(start + i * piece, piece), piece)
            there = pl.ds(pl.multiple_of(i * piece, piece), piece)
            total = res[at, q, core, span].astype(f32) + from_core[at, q, span].astype(f32)
            for term in terms:
                total = total + term[at, there].astype(f32)
            res[at, q, core, span] = total.astype(jnp.bfloat16)
            return carry

        lax.fori_loop(0, count // piece, body, 0)

    def corner(at):
        give(at, 3).wait_recv()
        add(at, 3, 0, rows, [])
        back_low(at).start()
        back_high(at).start()

    def compute(at, q):
        picks, scales, chosen = [], [], []
        for lane in range(2):
            listed = tok[at, q, lane, pl.ds(rows, tall - rows), pl.ds(0, rows)].astype(f32)
            listing = lax.broadcasted_iota(jnp.int32, listed.shape, 0)

            def row_of(index):
                return jnp.sum(jnp.where(listing == index, listed, 0.0), axis=0, keepdims=True)

            weight = row_of(experts + column) + row_of(2 * experts + column)
            index = lax.broadcasted_iota(jnp.int32, (capacity, rows), 0).astype(jnp.float32)
            hit = index == row_of(column)
            scales.append(jnp.sum(jnp.where(hit, weight, 0.0), axis=1, keepdims=True))
            picks.append(jnp.where(hit, 1.0, 0.0).astype(jnp.bfloat16))
            chosen.append(
                jnp.dot(picks[lane], tok[at, q, lane, pl.ds(0, rows)], preferred_element_type=jnp.float32)
                .astype(jnp.bfloat16)
            )
        gathered = jnp.concatenate(chosen, axis=0)
        gate_part = jnp.dot(gathered, gate_ref[...], preferred_element_type=jnp.float32)
        up_part = jnp.dot(gathered, up_ref[...], preferred_element_type=jnp.float32)
        hidden = (gate_part / (1.0 + jnp.exp(-gate_part)) * up_part).astype(jnp.bfloat16)
        partial = jnp.dot(hidden, down_ref[...], preferred_element_type=jnp.float32)
        partial = (partial * jnp.concatenate(scales, axis=0)).astype(jnp.bfloat16)
        for lane in range(2):
            res[at, q, lane] = lax.dot_general(
                picks[lane], partial[lane * capacity : (lane + 1) * capacity],
                (((0,), (0,)), ((), ())), preferred_element_type=jnp.float32,
            ).astype(jnp.bfloat16)

    def stage(turn, carry):
        @pl.when(turn < depth)
        def _():
            at = level_of(turn)
            pl.when(at < level)(lambda: up(at).wait_recv())
            pl.when(at > level)(lambda: down(at).wait_recv())
            pl.when((at <= level) & has_above)(lambda: up(at).start())
            pl.when((at >= level) & has_below)(lambda: down(at).start())
            to_right(at).start()
            to_left(at).start()
            share(at, 0).start()

        @pl.when((turn >= 1) & (turn < depth + 1))
        def _():
            at = level_of(turn - 1)
            to_right(at).wait_recv()
            on_right(at).start()
            share(at, 1).start()
            to_left(at).wait_recv()
            on_left(at).start()
            share(at, 2).start()

        @pl.when((turn >= 2) & (turn < depth + 2))
        def _():
            at = level_of(turn - 2)
            on_right(at).wait_recv()
            on_left(at).wait_recv()
            share(at, 3).start()

        pl.when(turn >= 3)(lambda: corner(level_of(turn - 3)))

        def one(q, inner):
            step = turn - (q + 1) // 2

            @pl.when((step >= 0) & (step < depth))
            def _():
                at = level_of(step)
                shared_in(at, q).wait_recv()
                compute(at, q)
                give(at, q).start()

            return inner

        lax.fori_loop(0, 4, one, 0)
        return carry

    lax.fori_loop(0, depth + 3, stage, 0)

    def extend(at, term):
        def body(i, carry):
            span = pl.ds(pl.multiple_of(i * piece, piece), piece)
            res[at, 0, core, span] = (
                res[at, 0, core, span].astype(f32) + term[at, span].astype(f32)
            ).astype(jnp.bfloat16)
            return carry

        lax.fori_loop(0, rows // piece, body, 0)

    def sides(at):
        give(at, 1).wait_recv()
        back_low(at).wait_recv()
        add(at, 1, 0, half, [half_low])
        add(at, 1, half, half, [])
        back_left(at).start()
        give(at, 2).wait_recv()
        back_high(at).wait_recv()
        add(at, 2, 0, half, [])
        add(at, 2, half, half, [half_high])
        back_right(at).start()

    def home(at):
        give(at, 0).wait_recv()
        back_left(at).wait_recv()
        back_right(at).wait_recv()
        add(at, 0, 0, rows, [from_right, from_left])

        @pl.when((at <= level) & has_above)
        def _():
            back_down(at).wait_recv()
            extend(at, from_above)

        @pl.when((at >= level) & has_below)
        def _():
            back_up(at).wait_recv()
            extend(at, from_below)

        pl.when(at < level)(lambda: back_down(at).start())
        pl.when(at > level)(lambda: back_up(at).start())

    def finish(turn, carry):
        pl.when(turn < depth - 1)(lambda: sides(level_of(depth - 1 - turn)))
        pl.when(turn >= 1)(lambda: home(level_of(depth - turn)))
        return carry

    sides(level)
    lax.fori_loop(0, depth + 1, finish, 0)
    out_copy = pltpu.make_async_copy(res.at[level, 0, core], out_ref, local_sem)
    out_copy.start()

    def drain(at, carry):
        pl.when((at <= level) & has_above)(lambda: up(at).wait_send())
        pl.when((at >= level) & has_below)(lambda: down(at).wait_send())
        for copy in (to_right, to_left, on_right, on_left):
            copy(at).wait_send()
        for copy in (back_low, back_high, back_left, back_right):
            copy(at).wait_send()
        for q in range(4):
            share(at, q).wait_send()
            give(at, q).wait_send()
        pl.when(at < level)(lambda: back_down(at).wait_send())
        pl.when(at > level)(lambda: back_up(at).wait_send())
        return carry

    lax.fori_loop(0, depth, drain, 0)
    out_copy.wait()


def dense_plan(expert_input, expert_gain, routes, route_weight, w_gate, w_up, w_down):
    row_count, width = expert_input.shape
    experts = lax.axis_size("ep")
    depth = lax.axis_size("tp") // 2
    capacity = 3 * routes.shape[1] * row_count // (2 * experts)
    normed = normalize(expert_input, expert_gain)
    listed = slots(routes, route_weight, experts)
    pad = -(-3 * experts // 16) * 16
    listed = jnp.pad(listed, ((0, pad - 3 * experts), (0, width - row_count)))
    sent = jnp.concatenate([normed, listed], axis=0)
    bf16 = jnp.bfloat16
    half = row_count // 2
    vmem = pl.BlockSpec(memory_space=pltpu.VMEM)
    return pl.pallas_call(
        functools.partial(stream_kernel, depth, capacity, experts),
        out_shape=jax.ShapeDtypeStruct((row_count, width), bf16),
        in_specs=[vmem] * 4,
        out_specs=vmem,
        scratch_shapes=[
            pltpu.VMEM((depth, 4, 2, row_count + pad, width), bf16),
            pltpu.VMEM((depth, 4, 2, row_count, width), bf16),
            pltpu.VMEM((depth, 4, row_count, width), bf16),
            pltpu.VMEM((depth, half, width), bf16),
            pltpu.VMEM((depth, half, width), bf16),
            pltpu.VMEM((depth, row_count, width), bf16),
            pltpu.VMEM((depth, row_count, width), bf16),
            pltpu.VMEM((depth, row_count, width), bf16),
            pltpu.VMEM((depth, row_count, width), bf16),
            pltpu.SemaphoreType.DMA((20, depth)),
            pltpu.SemaphoreType.DMA((20, depth)),
            pltpu.SemaphoreType.DMA,
        ],
        compiler_params=pltpu.CompilerParams(
            collective_id=0, has_side_effects=True, vmem_limit_bytes=60 * 2**20
        ),
    )(sent, w_gate[0], w_up[0], w_down[0])


def on_device(
    mixer_input, mixer_gain, group_weight, mixer_scale,
    expert_input, expert_gain, routes, route_weight, w_gate, w_up, w_down,
):
    devices = lax.axis_size(("ep", "tp"))
    gathered_bytes = 2 * devices * expert_input.size
    square = lax.axis_size("ep") == 4
    plan = dense_plan if square and gathered_bytes <= vmem_share else routed_plan
    expert_out = plan(expert_input, expert_gain, routes, route_weight, w_gate, w_up, w_down)
    return (mixer(mixer_input, mixer_gain, group_weight, mixer_scale), expert_out)


def solution(mesh):
    placed = (
        P(("ep", "tp"), None),
        P(),
        P(),
        P(),
        P(("ep", "tp"), None),
        P(),
        P(("ep", "tp"), None),
        P(("ep", "tp"), None),
        P("ep", None, "tp"),
        P("ep", None, "tp"),
        P("ep", "tp", None),
    )
    return jax.shard_map(
        on_device,
        mesh=mesh,
        in_specs=placed,
        out_specs=(P(("ep", "tp"), None), P(("ep", "tp"), None)),
        check_vma=False,
    )
```
